32 devices in a mesh: grp: 2 (over y), ep: 4 (over z), tp: 4 (over x, core).
Axes of the slice: x: 2, y: 2, z: 4, core: 2. Of those that a mesh axis runs over, the one named last changes fastest.
Arguments:
- outer_gate: bfloat16 [4096, 1024], P(('grp', 'ep'), 'tp'), parts along dimension 0, may hold values from -6 to 6
- inner_gate: bfloat16 [4096, 1024], P(('grp', 'ep'), 'tp'), parts along dimension 0, may hold values from -6 to 6
- conv_input: bfloat16 [4096, 1024], P(('grp', 'ep'), 'tp'), parts along dimension 0, may hold values from -6 to 6
- conv_taps: float32 [3, 1024], P(None, 'tp'), may hold values from -3.5 to 3.5
- mixer_weight: bfloat16 [1024, 2048], P('tp'), may hold values from -0.1875 to 0.1875
- expert_input: bfloat16 [4096, 2048], P(('grp', 'ep', 'tp')), parts along dimension 0, may hold values from -6 to 6
- norm_gain: float32 [2048], replicated, may hold values from 0.1 to 1.9
- expert_ids: int32 [4096, 2], P(('grp', 'ep', 'tp')), parts along dimension 0, may hold values from 0 to 3, all different within a row; in each aligned block of 128 rows (0 to 127, 128 to 255, ...) at most 80 rows name the same one
- route_weight: float32 [4096, 2], P(('grp', 'ep', 'tp')), parts along dimension 0, may hold values from 0.25 to 1
- gate_weight: bfloat16 [4, 2048, 3072], P('ep', None, 'tp'), may hold values from -0.125 to 0.125
- up_weight: bfloat16 [4, 2048, 3072], P('ep', None, 'tp'), may hold values from -0.125 to 0.125
- down_weight: bfloat16 [4, 3072, 2048], P('ep', 'tp'), may hold values from -0.109375 to 0.109375
Outputs:
- mixer_output: bfloat16 [4096, 2048], P(('grp', 'ep', 'tp')), parts along dimension 0
- expert_output: bfloat16 [4096, 2048], P(('grp', 'ep', 'tp')), parts along dimension 0
The draws below stay inside these ranges and needn't reach their ends.
There are 2 independent parts, one for each index of `grp`. The reference program is written for one: setup_inputs(seed, part) draws one part's arguments, and reference() takes and returns one part's arrays. A program takes and returns all parts, laid end to end along the dimension named above; an argument that names none is the same for every part. Nothing has to cross between parts.
Inputs may be any that keep to these rules, and one draw needn't show every extreme that they name: `expert_ids`: each row names 2 different experts. Among the rows of one device no expert is named more than 80 times, a bound that some block reaches.
All inputs are finite; a program needn't handle non-finite values.
Results may differ from the reference program's by a relative error of at most 0.011.
Values may be sent and summed in bfloat16 or wider, within the bound.
A program may use at most 128 MiB of HBM per device.

```python
import math
import jax
import jax.numpy as jnp
import numpy as np
from jax import lax

D = 2048
CONV_W = 1024
TAPS = 3
FF_E = 3072
TOP = 2
TOK_DEV = 128
EXPERTS = 4
CAP = 80
TOKENS = 2048
N_EP = 4
N_TP = 4


def level_of(key, shape, cuts, low, largest):
    gain = 1.0
    for dim, parts in cuts:
        heights = jax.random.uniform(jax.random.fold_in(jax.random.fold_in(key, 6), dim), (parts,), jnp.float32, low / len(cuts), largest / len(cuts))
        gain = gain * jnp.repeat(jnp.exp(heights), shape[dim] // parts).reshape((-1,) + (1,) * (len(shape) - 1 - dim))
    return gain


def deal_out(key, own, number, rows, number_of, top, limit, slope):
    ranking = jax.random.permutation(key, number_of)
    packed, common = shares(number_of, rows * top, limit, slope, True), shares(number_of, rows * top, limit, slope, False)
    places = jnp.arange(number_of)

    def named(lengths, rotation):
        used = int((lengths > 0).sum())
        fixed = max(1, used // 4)
        moved = fixed + (places - fixed + rotation * (used - fixed)) % max(1, number_of - fixed)
        return jnp.zeros((number_of,), jnp.int32).at[ranking[jnp.where(places < fixed, places, moved)]].set(jnp.asarray(lengths, jnp.int32))

    lengths = jnp.where(number % 4 == 0, named(packed, number // 4), named(common, number - number // 4 - 1))
    mixed = jax.random.permutation(jax.random.fold_in(own, 3), number_of)
    source_of, taker = mixed[0:number_of // 2 * 2:2], mixed[1:number_of // 2 * 2:2]
    margin = jnp.minimum(lengths[source_of] - 1, limit - lengths[taker]) // 2
    margin = jnp.where((source_of == ranking[0]) | (taker == ranking[0]) | (lengths[taker] == 0), 0, jnp.maximum(margin, 0))
    moved = jax.random.randint(jax.random.fold_in(own, 4), (number_of // 2,), 0, 1 << 20) % (margin + 1)
    lengths = lengths.at[source_of].add(-moved).at[taker].add(moved)
    members = jnp.searchsorted(jnp.cumsum(lengths), jnp.arange(rows * top), side="right").astype(jnp.int32)
    table = members.reshape(top, rows).T
    table = table[jax.random.permutation(jax.random.fold_in(own, 1), rows)]
    rotation = jax.random.randint(jax.random.fold_in(own, 2), (rows, 1), 0, top)
    return jnp.take_along_axis(table, (jnp.arange(top)[None, :] + rotation) % top, axis=1)


def shares(number_of, total, reach, skew, full):
    portions = [(1 << 20) // math.isqrt(rank ** skew) + 1 for rank in range(1, number_of + 1)]
    largest = reach if full else min(reach, max(-(-total // number_of), total * portions[0] // sum(portions)))
    least = 1 if total - largest >= number_of - 1 else 0
    given, rest = [largest] + [least] * (number_of - 1), total - largest - least * (number_of - 1)
    while rest > 0:
        candidates = [i for i in range(1, number_of) if given[i] < largest] or [i for i in range(1, number_of) if given[i] < reach]
        mass, budget = sum([portions[i] for i in candidates]), rest
        for i in candidates:
            extra = min(reach - given[i], max(1, budget * portions[i] // mass), rest)
            given[i] = given[i] + extra
            rest = rest - extra
    return np.array(given)


def normal_values(stream_key, extent, width, most, split=(), kind=jnp.bfloat16):
    entries = width * jax.random.normal(stream_key, extent, jnp.float32)
    if split:
        entries = entries * level_of(stream_key, extent, split, -0.22, 0.18)
    return jnp.clip(entries, -most, most).astype(kind)


def setup_inputs(seed: int = 0, part: int = 0) -> dict:
    key_of = jax.random.split(jax.random.key(seed), 13)
    part_keys = jax.random.split(jax.random.fold_in(key_of[12], part), 13)
    outer_gate = normal_values(part_keys[0], (TOKENS, CONV_W), 1.0, 6.0, ((0, 4), (1, 4)))
    inner_gate = normal_values(part_keys[1], (TOKENS, CONV_W), 1.0, 6.0, ((0, 4), (1, 4)))
    conv_input = normal_values(part_keys[2], (TOKENS, CONV_W), 1.0, 6.0, ((0, 4), (1, 4)))
    conv_taps = normal_values(key_of[3], (TAPS, CONV_W), TAPS ** -0.5, 3.5, ((1, 4),), jnp.float32)
    mixer_weight = normal_values(key_of[4], (CONV_W, D), CONV_W ** -0.5, 0.1875, ((0, 4),))
    expert_input = normal_values(part_keys[5], (TOKENS, D), 1.0, 6.0, ((0, 16),))
    norm_gain = jnp.clip(1.0 + 0.18 * jax.random.normal(key_of[6], (D,), jnp.float32), 0.1, 1.9)
    expert_ids_keys = jax.random.split(jax.random.fold_in(part_keys[7], 1), TOKENS // TOK_DEV)
    expert_ids_turns = jax.random.permutation(jax.random.fold_in(part_keys[7], 3), TOKENS // TOK_DEV)
    expert_ids = jax.vmap(lambda own, number: deal_out(jax.random.fold_in(part_keys[7], 2), own, number, TOK_DEV, EXPERTS, TOP, CAP, 1))(expert_ids_keys, expert_ids_turns).reshape((TOKENS, TOP))
    route_weight = jnp.clip(jnp.exp(math.log(1.0) - 1.3862944 * jax.random.uniform(part_keys[8], (TOKENS, TOP), jnp.float32) ** level_of(part_keys[8], (TOKENS, TOP), ((0, 16),), -0.2, 0.2)), 0.25, 1.0)
    gate_weight = normal_values(key_of[9], (EXPERTS, D, FF_E), D ** -0.5, 0.125, ((0, 4), (2, 4)))
    up_weight = normal_values(key_of[10], (EXPERTS, D, FF_E), D ** -0.5, 0.125, ((0, 4), (2, 4)))
    down_weight = normal_values(key_of[11], (EXPERTS, FF_E, D), FF_E ** -0.5, 0.109375, ((0, 4), (1, 4)))
    return {"outer_gate": outer_gate, "inner_gate": inner_gate, "conv_input": conv_input, "conv_taps": conv_taps, "mixer_weight": mixer_weight, "expert_input": expert_input, "norm_gain": norm_gain, "expert_ids": expert_ids, "route_weight": route_weight, "gate_weight": gate_weight, "up_weight": up_weight, "down_weight": down_weight}


epsilon = 1e-06

def rounded_sum(operand, weights, pieces):
    slice_width = operand.shape[1] // pieces
    summed = jnp.zeros((operand.shape[0], weights.shape[1]), jnp.float32)
    for piece_index in range(pieces):
        lower = piece_index * slice_width
        partial_value = jnp.dot(operand[:, lower:lower + slice_width], weights[lower:lower + slice_width], preferred_element_type=jnp.float32)
        summed = summed + lax.optimization_barrier(partial_value.astype(jnp.bfloat16)).astype(jnp.float32)
    return summed.astype(jnp.bfloat16)

def reference(outer_gate, inner_gate, conv_input, conv_taps, mixer_weight, expert_input, norm_gain, expert_ids, route_weight, gate_weight, up_weight, down_weight):
    gated_rows = inner_gate.astype(jnp.float32) * conv_input.astype(jnp.float32)
    length = gated_rows.shape[0]
    padded = jnp.pad(gated_rows, ((TAPS - 1, 0), (0, 0)))
    convolved = jnp.zeros_like(gated_rows)
    for tap_index in range(TAPS):
        convolved = convolved + conv_taps[tap_index] * padded[tap_index:tap_index + length]
    mixed = (outer_gate.astype(jnp.float32) * convolved).astype(jnp.bfloat16)
    mixer_output = rounded_sum(mixed, mixer_weight, N_TP)
    inputs = expert_input.astype(jnp.float32)
    normed = (inputs * lax.rsqrt(lax.optimization_barrier(jnp.mean(inputs * inputs, axis=1, keepdims=True)) + epsilon) * norm_gain).astype(jnp.bfloat16)
    flat_ids = expert_ids.reshape(-1)
    flat_weights = route_weight.reshape(-1)
    most_rows = N_EP * N_TP * CAP

    def one_expert(expert):
        chosen = flat_ids == expert
        picked = jnp.nonzero(chosen, size=most_rows, fill_value=0)[0].astype(jnp.int32)
        valid = jnp.arange(most_rows, dtype=jnp.int32) < jnp.sum(chosen.astype(jnp.int32))
        owners = (picked // TOP).astype(jnp.int32)
        token_rows = normed[owners]
        gate_value = jnp.dot(token_rows, gate_weight[expert], preferred_element_type=jnp.float32)
        up_value = jnp.dot(token_rows, up_weight[expert], preferred_element_type=jnp.float32)
        hidden = (jax.nn.silu(gate_value) * up_value).astype(jnp.bfloat16)
        answer = rounded_sum(hidden, down_weight[expert], N_TP)
        pair_weight = jnp.where(valid, flat_weights[picked], jnp.zeros_like(flat_weights[picked]))
        return (owners, answer.astype(jnp.float32) * pair_weight[:, None])
    owners, contributions = lax.map(one_expert, jnp.arange(EXPERTS, dtype=jnp.int32))
    summed = jax.ops.segment_sum(contributions.reshape(-1, D), owners.reshape(-1), num_segments=TOKENS)
    expert_output = summed.astype(jnp.bfloat16)
    return (mixer_output, expert_output)
```

```python
import functools

import jax
import jax.numpy as jnp
from jax import lax
from jax.experimental import pallas as pl
from jax.experimental.pallas import tpu as pltpu
from jax.sharding import PartitionSpec as P

EPSILON = 1e-06
F32 = jnp.float32
BF16 = jnp.bfloat16
MESH = pl.DeviceIdType.MESH
HALO = 8


def round_up(value, multiple):
    return (value + multiple - 1) // multiple * multiple


def add(*values):
    total = values[0].astype(F32)
    for value in values[1:]:
        total = total + value.astype(F32)
    return total.astype(BF16)


def kernel(
    n_ep,
    n_tp,
    cap,
    outer_ref,
    inner_ref,
    conv_ref,
    taps_ref,
    mixer_hbm,
    x_ref,
    gain_ref,
    ids_ref,
    ids_t_ref,
    route_ref,
    gate_hbm,
    up_hbm,
    down_hbm,
    mixer_out,
    expert_out,
    mixer_w,
    gate_w,
    up_w,
    down_w,
    normed,
    outbox,
    rows,
    part,
    core_in,
    chip_sum,
    cross_in,
    ret,
    ans,
    hid,
    gated,
    halo,
    mixed,
    m_part,
    m_core_in,
    m_chip_sum,
    m_cross_in,
    w_sem,
    z_send,
    z_recv,
    core_send,
    g_recv,
    cross_send,
    a_send,
    a_recv,
    b_send,
    b_recv,
    r_send,
    r_recv,
    h_sem,
    m_sem,
):
    half = n_tp // 2
    me = lax.axis_index("ep")
    t = lax.axis_index("tp")
    c = lax.rem(t, 2)
    a = t // 2
    pair = t + 1 - 2 * c
    others = [lax.rem(a + j, half) for j in range(1, half)]
    tokens, width = x_ref.shape
    length = inner_ref.shape[0]

    def source(i):
        if n_ep == 4:
            if i == 0:
                return me
            if i == 1:
                return me + 1 - 2 * lax.rem(me, 2)
            two = me + 2 - 4 * (me // 2)
            three = 3 - me
            inside = lax.rem((me + 1) // 2, 2)
            if i == 2:
                return two + inside * (three - two)
            return three + inside * (two - three)
        return lax.rem(me + i, n_ep)

    def remote(src, dst, send, recv, **where):
        return pltpu.make_async_remote_copy(
            src_ref=src,
            dst_ref=dst,
            send_sem=send,
            recv_sem=recv,
            device_id=where,
            device_id_type=MESH,
        )

    loads = [
        pltpu.make_async_copy(src, dst, w_sem.at[i])
        for i, (src, dst) in enumerate(
            [
                (mixer_hbm, mixer_w),
                (gate_hbm.at[0], gate_w),
                (up_hbm.at[0], up_w),
                (down_hbm.at[0], down_w),
            ]
        )
    ]
    for load in loads:
        load.start()

    barrier = pltpu.get_barrier_semaphore()
    for j in range(1, n_ep):
        pl.semaphore_signal(
            barrier, inc=1, device_id={"ep": lax.rem(me + j, n_ep)}, device_id_type=MESH
        )
    for j in range(1, n_tp):
        pl.semaphore_signal(
            barrier, inc=1, device_id={"tp": lax.rem(t + j, n_tp)}, device_id_type=MESH
        )

    values = x_ref[...].astype(F32)
    scale = lax.rsqrt(jnp.mean(values * values, axis=1, keepdims=True) + EPSILON)
    normed[...] = (values * scale * gain_ref[...]).astype(BF16)
    e_rows = round_up(n_ep, 8)
    e_iota = lax.broadcasted_iota(jnp.int32, (e_rows, tokens), 0)
    first, second = ids_t_ref[0:1, :], ids_t_ref[1:2, :]
    is_first, is_second = e_iota == first, e_iota == second
    named = jnp.where(is_first | is_second, 1.0, 0.0).astype(BF16)
    row_i = lax.broadcasted_iota(jnp.int32, (tokens, tokens), 0)
    col_i = lax.broadcasted_iota(jnp.int32, (tokens, tokens), 1)
    before = jnp.where(row_i < col_i, 1.0, 0.0).astype(BF16)
    rank = jnp.dot(named, before, preferred_element_type=F32)
    rank_1 = jnp.sum(jnp.where(is_first, rank, 0.0), axis=0, keepdims=True)
    rank_2 = jnp.sum(jnp.where(is_second, rank, 0.0), axis=0, keepdims=True)
    slot_1 = first.astype(F32) * cap + rank_1
    slot_2 = second.astype(F32) * cap + rank_2
    slots = lax.broadcasted_iota(jnp.int32, (n_ep * cap, tokens), 0).astype(F32)
    pack = jnp.where((slots == slot_1) | (slots == slot_2), 1.0, 0.0).astype(BF16)
    tile = 512
    for n in range(width // tile):
        cols = slice(n * tile, (n + 1) * tile)
        packed = jnp.dot(pack, normed[:, cols], preferred_element_type=F32)
        outbox[:, :, cols] = packed.astype(BF16).reshape(n_ep, cap, tile)

    gated[HALO:, :] = inner_ref[...].astype(F32) * conv_ref[...].astype(F32)

    pl.semaphore_wait(barrier, n_ep - 1 + n_tp - 1)

    nxt = lax.rem(me + 1, n_ep)
    halo_copy = remote(
        gated.at[pl.ds(length, HALO)], halo, h_sem.at[0], h_sem.at[1], ep=nxt
    )
    halo_copy.start()

    def dispatch(i):
        d = source(i)
        return remote(
            outbox.at[d], rows.at[me, t], z_send.at[d], z_recv.at[me], ep=d
        )

    def own_to_pair(s):
        return remote(
            rows.at[s, t], rows.at[s, t], core_send.at[s, t], g_recv.at[s, t], tp=pair
        )

    def own_to_cross(s, o):
        return remote(
            rows.at[s, t], rows.at[s, t], cross_send.at[s, o], g_recv.at[s, t], tp=2 * o + c
        )

    def cross_to_pair(s, o):
        q = 2 * o + c
        return remote(
            rows.at[s, q], rows.at[s, q], core_send.at[s, q], g_recv.at[s, q], tp=pair
        )

    def arrival(s, q):
        return remote(
            rows.at[s, q], rows.at[s, q], core_send.at[s, q], g_recv.at[s, q], tp=pair
        )

    def spread(s):
        for o in others:
            own_to_cross(s, o).start()
        own_to_pair(s).start()

    def pre(i):
        s = source(i)
        remote(outbox.at[s], rows.at[s, t], z_send.at[s], z_recv.at[s], ep=s).wait_recv()
        spread(s)

    def loop(lower, upper, body):
        if upper - lower <= 4:
            for i in range(lower, upper):
                body(i)
        else:
            lax.fori_loop(lower, upper, lambda i, _: (body(i), 0)[1], 0)

    rows[me, t] = outbox[me]
    spread(me)
    loop(1, n_ep, lambda i: dispatch(i).start())

    halo_copy.wait_recv()
    kept = jnp.where(me > 0, 1.0, 0.0)
    gated[0:HALO, :] = halo[...] * kept
    count = taps_ref.shape[0]
    convolved = jnp.zeros((length, gated.shape[1]), F32)
    for k in range(count):
        lower = HALO - (count - 1) + k
        convolved = convolved + taps_ref[k : k + 1, :] * gated[lower : lower + length, :]
    mixed[...] = (outer_ref[...].astype(F32) * convolved).astype(BF16)
    loads[0].wait()

    def mixer_tile(n, _):
        cols = pl.ds(pl.multiple_of(n * tile, tile), tile)
        for q in range(n_tp):
            value = jnp.dot(
                mixed[q * tokens : (q + 1) * tokens, :],
                mixer_w[:, cols],
                preferred_element_type=F32,
            )
            m_part[q % 2, q // 2, :, cols] = value.astype(BF16)
        return 0

    lax.fori_loop(0, width // tile, mixer_tile, 0)
    m_core = remote(m_part.at[1 - c], m_core_in, m_sem.at[0], m_sem.at[1], tp=pair)
    m_core.start()

    def m_cross(o):
        return remote(
            m_chip_sum.at[o],
            m_cross_in.at[a],
            m_sem.at[2 + o],
            m_sem.at[2 + half + a],
            tp=2 * o + c,
        )

    m_core.wait_recv()
    for o in others:
        m_chip_sum[o] = add(m_part[c, o], m_core_in[o])
        m_cross(o).start()

    def mixer_finish():
        for o in others:
            remote(
                m_chip_sum.at[o],
                m_cross_in.at[o],
                m_sem.at[2 + o],
                m_sem.at[2 + half + o],
                tp=2 * o + c,
            ).wait_recv()
        mixer_out[...] = add(
            m_part[c, a], m_core_in[a], *[m_cross_in[o] for o in others]
        )

    def gathered(i):
        s = source(i)
        for o in others:
            arrival(s, 2 * o + c).wait_recv()
            cross_to_pair(s, o).start()
        for o in range(half):
            arrival(s, 2 * o + 1 - c).wait_recv()

    f_tile = 256

    def compute(i):
        s = source(i)

        def up_tile(n, _):
            cols = pl.ds(pl.multiple_of(n * f_tile, f_tile), f_tile)
            block = rows[s].reshape(n_tp * cap, width)
            g = jnp.dot(block, gate_w[:, cols], preferred_element_type=F32)
            u = jnp.dot(block, up_w[:, cols], preferred_element_type=F32)
            hid[:, cols] = (g / (1.0 + jnp.exp(-g)) * u).astype(BF16)
            return 0

        lax.fori_loop(0, hid.shape[1] // f_tile, up_tile, 0)

        def down_tile(n, _):
            cols = pl.ds(pl.multiple_of(n * tile, tile), tile)
            value = jnp.dot(hid[...], down_w[:, cols], preferred_element_type=F32)
            value = value.astype(BF16).reshape(n_tp, cap, tile)
            for q in range(n_tp):
                part[s, q % 2, q // 2, :, cols] = value[q]
            return 0

        lax.fori_loop(0, width // tile, down_tile, 0)
        to_pair(s).start()

    def to_pair(s):
        return remote(
            part.at[s, 1 - c], core_in.at[s], a_send.at[s], a_recv.at[s], tp=pair
        )

    def to_cross(s, o):
        return remote(
            chip_sum.at[s, o], cross_in.at[s, a], b_send.at[s, o], b_recv.at[s, a], tp=2 * o + c
        )

    def middle(i):
        s = source(i)
        to_pair(s).wait_recv()
        for o in others:
            chip_sum[s, o] = add(part[s, c, o], core_in[s, o])
            to_cross(s, o).start()

    def give_back(s):
        return remote(ret.at[s], ans.at[me], r_send.at[s], r_recv.at[me], ep=s)

    def finish(i, own=False):
        s = source(i)
        for o in others:
            remote(
                chip_sum.at[s, o], cross_in.at[s, o], b_send.at[s, o], b_recv.at[s, o], tp=2 * o + c
            ).wait_recv()
        total = add(part[s, c, a], core_in[s, a], *[cross_in[s, o] for o in others])
        if own:
            ans[s] = total
        else:
            ret[s] = total
            give_back(s).start()

    def step(i):
        pre(i + 1)
        gathered(i)
        compute(i)
        finish(i - 1)
        middle(i)

    for load in loads[1:]:
        load.wait()
    pre(1)
    gathered(0)
    compute(0)
    middle(0)
    mixer_finish()
    pre(2)
    gathered(1)
    compute(1)
    finish(0, own=True)
    middle(1)
    loop(2, n_ep - 1, step)
    gathered(n_ep - 1)
    compute(n_ep - 1)
    finish(n_ep - 2)
    middle(n_ep - 1)
    finish(n_ep - 1)

    lanes = 128
    l_iota = lax.broadcasted_iota(jnp.int32, (tokens, lanes), 1)
    id_1, id_2 = ids_ref[:, 0:1], ids_ref[:, 1:2]
    l_first, l_second = l_iota == id_1, l_iota == id_2
    l_named = jnp.where(l_first | l_second, 1.0, 0.0).astype(BF16)
    after = jnp.where(col_i < row_i, 1.0, 0.0).astype(BF16)
    l_rank = jnp.dot(after, l_named, preferred_element_type=F32)
    p_1 = id_1.astype(F32) * cap + jnp.sum(
        jnp.where(l_first, l_rank, 0.0), axis=1, keepdims=True
    )
    p_2 = id_2.astype(F32) * cap + jnp.sum(
        jnp.where(l_second, l_rank, 0.0), axis=1, keepdims=True
    )
    places = lax.broadcasted_iota(jnp.int32, (tokens, n_ep * cap), 1).astype(F32)
    weight = jnp.where(places == p_1, route_ref[:, 0:1], 0.0) + jnp.where(
        places == p_2, route_ref[:, 1:2], 0.0
    )
    high = weight.astype(BF16)
    low = (weight - high.astype(F32)).astype(BF16)

    def answer_in(i):
        e = source(i)
        remote(ret.at[e], ans.at[e], r_send.at[e], r_recv.at[e], ep=e).wait_recv()

    loop(1, n_ep, answer_in)

    def combine_tile(n, _):
        cols = pl.ds(pl.multiple_of(n * tile, tile), tile)
        block = ans[:, :, cols].reshape(n_ep * cap, tile)
        expert_out[:, cols] = (
            jnp.dot(high, block, preferred_element_type=F32)
            + jnp.dot(low, block, preferred_element_type=F32)
        ).astype(BF16)
        return 0

    lax.fori_loop(0, width // tile, combine_tile, 0)

    halo_copy.wait_send()
    m_core.wait_send()
    for o in others:
        m_cross(o).wait_send()

    def drain(i):
        s = source(i)
        for o in others:
            own_to_cross(s, o).wait_send()
            cross_to_pair(s, o).wait_send()
            to_cross(s, o).wait_send()
        own_to_pair(s).wait_send()
        to_pair(s).wait_send()

    def drain_far(i):
        dispatch(i).wait_send()
        give_back(source(i)).wait_send()

    loop(0, n_ep, drain)
    loop(1, n_ep, drain_far)


def on_device(
    n_ep,
    n_tp,
    outer_gate,
    inner_gate,
    conv_input,
    conv_taps,
    mixer_weight,
    expert_input,
    norm_gain,
    expert_ids,
    route_weight,
    gate_weight,
    up_weight,
    down_weight,
):
    tokens, width = expert_input.shape
    top = expert_ids.shape[1]
    cap = round_up(5 * tokens * top // (4 * n_ep), 16)
    half = n_tp // 2
    length, channels = inner_gate.shape
    hidden = gate_weight.shape[2]
    vmem = pl.BlockSpec(memory_space=pltpu.VMEM)
    hbm = pl.BlockSpec(memory_space=pl.ANY)
    dma = pltpu.SemaphoreType.DMA
    v = pltpu.VMEM
    out = jax.ShapeDtypeStruct((tokens, width), BF16)
    return pl.pallas_call(
        functools.partial(kernel, n_ep, n_tp, cap),
        out_shape=(out, out),
        in_specs=[vmem] * 4 + [hbm] + [vmem] * 5 + [hbm] * 3,
        out_specs=(vmem, vmem),
        scratch_shapes=[
            v(mixer_weight.shape, BF16),
            v(gate_weight.shape[1:], BF16),
            v(up_weight.shape[1:], BF16),
            v(down_weight.shape[1:], BF16),
            v((tokens, width), BF16),
            v((n_ep, cap, width), BF16),
            v((n_ep, n_tp, cap, width), BF16),
            v((n_ep, 2, half, cap, width), BF16),
            v((n_ep, half, cap, width), BF16),
            v((n_ep, half, cap, width), BF16),
            v((n_ep, half, cap, width), BF16),
            v((n_ep, cap, width), BF16),
            v((n_ep, cap, width), BF16),
            v((n_tp * cap, hidden), BF16),
            v((HALO + length, channels), F32),
            v((HALO, channels), F32),
            v((length, channels), BF16),
            v((2, half, tokens, width), BF16),
            v((half, tokens, width), BF16),
            v((half, tokens, width), BF16),
            v((half, tokens, width), BF16),
            dma((4,)),
            dma((n_ep,)),
            dma((n_ep,)),
            dma((n_ep, n_tp)),
            dma((n_ep, n_tp)),
            dma((n_ep, half)),
            dma((n_ep,)),
            dma((n_ep,)),
            dma((n_ep, half)),
            dma((n_ep, half)),
            dma((n_ep,)),
            dma((n_ep,)),
            dma((2,)),
            dma((2 + 2 * half,)),
        ],
        compiler_params=pltpu.CompilerParams(
            collective_id=0, has_side_effects=True, vmem_limit_bytes=60 * 1024 * 1024
        ),
    )(
        outer_gate,
        inner_gate,
        conv_input,
        conv_taps,
        mixer_weight,
        expert_input,
        norm_gain.reshape(1, -1),
        expert_ids,
        expert_ids.T,
        route_weight,
        gate_weight,
        up_weight,
        down_weight,
    )


def solution(mesh):
    return jax.shard_map(
        functools.partial(on_device, mesh.shape["ep"], mesh.shape["tp"]),
        mesh=mesh,
        in_specs=(
            P(("grp", "ep"), "tp"),
            P(("grp", "ep"), "tp"),
            P(("grp", "ep"), "tp"),
            P(None, "tp"),
            P("tp", None),
            P(("grp", "ep", "tp"), None),
            P(),
            P(("grp", "ep", "tp"), None),
            P(("grp", "ep", "tp"), None),
            P("ep", None, "tp"),
            P("ep", None, "tp"),
            P("ep", "tp", None),
        ),
        out_specs=(P(("grp", "ep", "tp"), None), P(("grp", "ep", "tp"), None)),
        check_vma=False,
    )
```

```python
import functools

import jax
import jax.numpy as jnp
from jax import lax
from jax.experimental import pallas as pl
from jax.experimental.pallas import tpu as pltpu
from jax.sharding import PartitionSpec as P

EPSILON = 1e-06
F32 = jnp.float32
BF16 = jnp.bfloat16
MESH = pl.DeviceIdType.MESH
HALO = 8


def round_up(value, multiple):
    return (value + multiple - 1) // multiple * multiple


def add(*values):
    total = values[0].astype(F32)
    for value in values[1:]:
        total = total + value.astype(F32)
    return total.astype(BF16)


def kernel(
    n_ep,
    n_tp,
    cap,
    outer_ref,
    inner_ref,
    conv_ref,
    taps_ref,
    mixer_hbm,
    x_ref,
    gain_ref,
    ids_ref,
    route_ref,
    gate_hbm,
    up_hbm,
    down_hbm,
    mixer_out,
    expert_out,
    mixer_w,
    gate_w,
    up_w,
    down_w,
    normed,
    weights,
    outbox,
    rows,
    part,
    core_in,
    chip_sum,
    cross_in,
    ret,
    ans,
    hid,
    gated,
    halo,
    mixed,
    m_part,
    m_core_in,
    m_chip_sum,
    m_cross_in,
    w_sem,
    z_send,
    z_recv,
    core_send,
    g_recv,
    cross_send,
    a_send,
    a_recv,
    b_send,
    b_recv,
    r_send,
    r_recv,
    h_sem,
    m_sem,
):
    half = n_tp // 2
    me = lax.axis_index("ep")
    t = lax.axis_index("tp")
    c = lax.rem(t, 2)
    a = t // 2
    pair = t + 1 - 2 * c
    others = [lax.rem(a + j, half) for j in range(1, half)]
    tokens, width = x_ref.shape
    length = inner_ref.shape[0]

    def departure(i):
        if n_ep == 4:
            if i == 0:
                return me
            two = me + 2 - 4 * (me // 2)
            if i == 1:
                return two
            one = me + 1 - 2 * lax.rem(me, 2)
            three = 3 - me
            inside = lax.rem((me + 1) // 2, 2)
            if i == 2:
                return one + inside * (three - one)
            return three + inside * (one - three)
        return lax.rem(me + i, n_ep)

    def source(i):
        if n_ep == 4:
            return [
                me,
                me + 2 - 4 * (me // 2),
                3 - me,
                me + 1 - 2 * lax.rem(me, 2),
            ][i]
        return lax.rem(me + i, n_ep)

    def remote(src, dst, send, recv, **where):
        return pltpu.make_async_remote_copy(
            src_ref=src,
            dst_ref=dst,
            send_sem=send,
            recv_sem=recv,
            device_id=where,
            device_id_type=MESH,
        )

    loads = [
        pltpu.make_async_copy(src, dst, w_sem.at[i])
        for i, (src, dst) in enumerate(
            [
                (mixer_hbm, mixer_w),
                (gate_hbm.at[0], gate_w),
                (up_hbm.at[0], up_w),
                (down_hbm.at[0], down_w),
            ]
        )
    ]
    for load in loads:
        load.start()

    barrier = pltpu.get_barrier_semaphore()
    for j in range(1, n_ep):
        pl.semaphore_signal(
            barrier, inc=1, device_id={"ep": lax.rem(me + j, n_ep)}, device_id_type=MESH
        )
    for j in range(1, n_tp):
        pl.semaphore_signal(
            barrier, inc=1, device_id={"tp": lax.rem(t + j, n_tp)}, device_id_type=MESH
        )

    values = x_ref[...].astype(F32)
    scale = lax.rsqrt(jnp.mean(values * values, axis=1, keepdims=True) + EPSILON)
    normed[...] = (values * scale * gain_ref[...]).astype(BF16)
    e_rows = round_up(n_ep, 8)
    e_iota = lax.broadcasted_iota(jnp.int32, (e_rows, tokens), 0)
    first, second = ids_ref[0:1, :], ids_ref[1:2, :]
    is_first, is_second = e_iota == first, e_iota == second
    named = jnp.where(is_first | is_second, 1.0, 0.0).astype(BF16)
    row_i = lax.broadcasted_iota(jnp.int32, (tokens, tokens), 0)
    col_i = lax.broadcasted_iota(jnp.int32, (tokens, tokens), 1)
    before = jnp.where(row_i < col_i, 1.0, 0.0).astype(BF16)
    rank = jnp.dot(named, before, preferred_element_type=F32)
    rank_1 = jnp.sum(jnp.where(is_first, rank, 0.0), axis=0, keepdims=True)
    rank_2 = jnp.sum(jnp.where(is_second, rank, 0.0), axis=0, keepdims=True)
    slot_1 = first.astype(F32) * cap + rank_1
    slot_2 = second.astype(F32) * cap + rank_2
    slots = lax.broadcasted_iota(jnp.int32, (n_ep * cap, tokens), 0).astype(F32)
    pack = jnp.where((slots == slot_1) | (slots == slot_2), 1.0, 0.0).astype(BF16)
    tile = 512
    for n in range(width // tile):
        cols = slice(n * tile, (n + 1) * tile)
        packed = jnp.dot(pack, normed[:, cols], preferred_element_type=F32)
        outbox[:, :, cols] = packed.astype(BF16).reshape(n_ep, cap, tile)

    gated[HALO:, :] = inner_ref[...].astype(F32) * conv_ref[...].astype(F32)

    pl.semaphore_wait(barrier, n_ep - 1 + n_tp - 1)

    nxt = lax.rem(me + 1, n_ep)
    halo_copy = remote(
        gated.at[pl.ds(length, HALO)], halo, h_sem.at[0], h_sem.at[1], ep=nxt
    )
    halo_copy.start()

    def dispatch(i):
        d = departure(i)
        return remote(
            outbox.at[d], rows.at[me, t], z_send.at[d], z_recv.at[me], ep=d
        )

    def own_to_pair(s):
        return remote(
            rows.at[s, t], rows.at[s, t], core_send.at[s, t], g_recv.at[s, t], tp=pair
        )

    def own_to_cross(s, o):
        return remote(
            rows.at[s, t], rows.at[s, t], cross_send.at[s, o], g_recv.at[s, t], tp=2 * o + c
        )

    def cross_to_pair(s, o):
        q = 2 * o + c
        return remote(
            rows.at[s, q], rows.at[s, q], core_send.at[s, q], g_recv.at[s, q], tp=pair
        )

    def arrival(s, q):
        return remote(
            rows.at[s, q], rows.at[s, q], core_send.at[s, q], g_recv.at[s, q], tp=pair
        )

    def spread(s):
        for o in others:
            own_to_cross(s, o).start()
        own_to_pair(s).start()

    def pre(i):
        s = source(i)
        remote(outbox.at[s], rows.at[s, t], z_send.at[s], z_recv.at[s], ep=s).wait_recv()
        spread(s)

    def loop(lower, upper, body):
        if upper - lower <= 4:
            for i in range(lower, upper):
                body(i)
        else:
            lax.fori_loop(lower, upper, lambda i, _: (body(i), 0)[1], 0)

    rows[me, t] = outbox[me]
    spread(me)
    loop(1, n_ep, lambda i: dispatch(i).start())

    halo_copy.wait_recv()
    kept = jnp.where(me > 0, 1.0, 0.0)
    gated[0:HALO, :] = halo[...] * kept
    count = taps_ref.shape[0]
    convolved = jnp.zeros((length, gated.shape[1]), F32)
    for k in range(count):
        lower = HALO - (count - 1) + k
        convolved = convolved + taps_ref[k : k + 1, :] * gated[lower : lower + length, :]
    mixed[...] = (outer_ref[...].astype(F32) * convolved).astype(BF16)
    loads[0].wait()

    def mixer_tile(n, _):
        cols = pl.ds(pl.multiple_of(n * tile, tile), tile)
        for q in range(n_tp):
            value = jnp.dot(
                mixed[q * tokens : (q + 1) * tokens, :],
                mixer_w[:, cols],
                preferred_element_type=F32,
            )
            m_part[q % 2, q // 2, :, cols] = value.astype(BF16)
        return 0

    lax.fori_loop(0, width // tile, mixer_tile, 0)
    m_core = remote(m_part.at[1 - c], m_core_in, m_sem.at[0], m_sem.at[1], tp=pair)
    m_core.start()

    piece = tokens // 2

    def m_cross(o, h, slot):
        return remote(
            m_chip_sum.at[o, pl.ds(h * piece, piece)],
            m_cross_in.at[slot, pl.ds(h * piece, piece)],
            m_sem.at[2 + 2 * o + h],
            m_sem.at[2 + n_tp + 2 * slot + h],
            tp=2 * o + c,
        )

    m_core.wait_recv()
    for o in others:
        m_chip_sum[o] = add(m_part[c, o], m_core_in[o])
        m_cross(o, 0, a).start()

    def mixer_rest():
        for o in others:
            m_cross(o, 1, a).start()

    def mixer_finish():
        for o in others:
            m_cross(o, 0, o).wait_recv()
            m_cross(o, 1, o).wait_recv()
        mixer_out[...] = add(
            m_part[c, a], m_core_in[a], *[m_cross_in[o] for o in others]
        )

    def gathered(i):
        s = source(i)
        for o in others:
            arrival(s, 2 * o + c).wait_recv()
            cross_to_pair(s, o).start()
        for o in range(half):
            arrival(s, 2 * o + 1 - c).wait_recv()

    f_tile = 256

    def compute(i):
        s = source(i)

        def up_tile(n, _):
            cols = pl.ds(pl.multiple_of(n * f_tile, f_tile), f_tile)
            block = rows[s].reshape(n_tp * cap, width)
            g = jnp.dot(block, gate_w[:, cols], preferred_element_type=F32)
            u = jnp.dot(block, up_w[:, cols], preferred_element_type=F32)
            hid[:, cols] = (g / (1.0 + jnp.exp(-g)) * u).astype(BF16)
            return 0

        lax.fori_loop(0, hid.shape[1] // f_tile, up_tile, 0)

        def down_tile(n, _):
            cols = pl.ds(pl.multiple_of(n * tile, tile), tile)
            value = jnp.dot(hid[...], down_w[:, cols], preferred_element_type=F32)
            value = value.astype(BF16).reshape(n_tp, cap, tile)
            for q in range(n_tp):
                part[s, q % 2, q // 2, :, cols] = value[q]
            return 0

        lax.fori_loop(0, width // tile, down_tile, 0)
        to_pair(s).start()

    def to_pair(s):
        return remote(
            part.at[s, 1 - c], core_in.at[s], a_send.at[s], a_recv.at[s], tp=pair
        )

    def to_cross(s, o):
        return remote(
            chip_sum.at[s, o], cross_in.at[s, a], b_send.at[s, o], b_recv.at[s, a], tp=2 * o + c
        )

    def middle(i):
        s = source(i)
        to_pair(s).wait_recv()
        for o in others:
            chip_sum[s, o] = add(part[s, c, o], core_in[s, o])
            to_cross(s, o).start()

    def give_back(s):
        return remote(ret.at[s], ans.at[me], r_send.at[s], r_recv.at[me], ep=s)

    def finish(i, own=False):
        s = source(i)
        for o in others:
            remote(
                chip_sum.at[s, o], cross_in.at[s, o], b_send.at[s, o], b_recv.at[s, o], tp=2 * o + c
            ).wait_recv()
        total = add(part[s, c, a], core_in[s, a], *[cross_in[s, o] for o in others])
        if own:
            ans[s] = total
        else:
            ret[s] = total
            give_back(s).start()

    def step(i):
        pre(i + 1)
        gathered(i)
        compute(i)
        finish(i - 1)
        middle(i)

    for load in loads[1:]:
        load.wait()
    pre(1)
    mixer_rest()
    gathered(0)
    compute(0)
    pre(2)
    gathered(1)
    compute(1)
    middle(1)
    loop(2, n_ep - 1, step)
    gathered(n_ep - 1)
    compute(n_ep - 1)
    finish(n_ep - 2)
    middle(n_ep - 1)
    middle(0)
    mixer_finish()

    weight = jnp.where(slots == slot_1, route_ref[0:1, :], 0.0) + jnp.where(
        slots == slot_2, route_ref[1:2, :], 0.0
    )
    weights[0] = weight.astype(BF16)
    weights[1] = (weight - weight.astype(BF16).astype(F32)).astype(BF16)
    finish(n_ep - 1)
    finish(0, own=True)

    def answer_in(i):
        e = source(i)
        remote(ret.at[e], ans.at[e], r_send.at[e], r_recv.at[e], ep=e).wait_recv()

    loop(1, n_ep, answer_in)

    def weighted(left, right):
        return lax.dot_general(
            left, right, (((0,), (0,)), ((), ())), preferred_element_type=F32
        )

    def combine_tile(n, _):
        cols = pl.ds(pl.multiple_of(n * tile, tile), tile)
        block = ans[:, :, cols].reshape(n_ep * cap, tile)
        expert_out[:, cols] = (
            weighted(weights[0], block) + weighted(weights[1], block)
        ).astype(BF16)
        return 0

    lax.fori_loop(0, width // tile, combine_tile, 0)

    halo_copy.wait_send()
    m_core.wait_send()
    for o in others:
        m_cross(o, 0, a).wait_send()
        m_cross(o, 1, a).wait_send()

    def drain(i):
        s = source(i)
        for o in others:
            own_to_cross(s, o).wait_send()
            cross_to_pair(s, o).wait_send()
            to_cross(s, o).wait_send()
        own_to_pair(s).wait_send()
        to_pair(s).wait_send()

    def drain_far(i):
        dispatch(i).wait_send()
        give_back(source(i)).wait_send()

    loop(0, n_ep, drain)
    loop(1, n_ep, drain_far)


def on_device(
    n_ep,
    n_tp,
    outer_gate,
    inner_gate,
    conv_input,
    conv_taps,
    mixer_weight,
    expert_input,
    norm_gain,
    expert_ids,
    route_weight,
    gate_weight,
    up_weight,
    down_weight,
):
    tokens, width = expert_input.shape
    top = expert_ids.shape[1]
    cap = round_up(5 * tokens * top // (4 * n_ep), 16)
    half = n_tp // 2
    length, channels = inner_gate.shape
    hidden = gate_weight.shape[2]
    vmem = pl.BlockSpec(memory_space=pltpu.VMEM)
    hbm = pl.BlockSpec(memory_space=pl.ANY)
    dma = pltpu.SemaphoreType.DMA
    v = pltpu.VMEM
    out = jax.ShapeDtypeStruct((tokens, width), BF16)
    return pl.pallas_call(
        functools.partial(kernel, n_ep, n_tp, cap),
        out_shape=(out, out),
        in_specs=[vmem] * 4 + [hbm] + [vmem] * 4 + [hbm] * 3,
        out_specs=(vmem, vmem),
        scratch_shapes=[
            v(mixer_weight.shape, BF16),
            v(gate_weight.shape[1:], BF16),
            v(up_weight.shape[1:], BF16),
            v(down_weight.shape[1:], BF16),
            v((tokens, width), BF16),
            v((2, n_ep * cap, tokens), BF16),
            v((n_ep, cap, width), BF16),
            v((n_ep, n_tp, cap, width), BF16),
            v((n_ep, 2, half, cap, width), BF16),
            v((n_ep, half, cap, width), BF16),
            v((n_ep, half, cap, width), BF16),
            v((n_ep, half, cap, width), BF16),
            v((n_ep, cap, width), BF16),
            v((n_ep, cap, width), BF16),
            v((n_tp * cap, hidden), BF16),
            v((HALO + length, channels), F32),
            v((HALO, channels), F32),
            v((length, channels), BF16),
            v((2, half, tokens, width), BF16),
            v((half, tokens, width), BF16),
            v((half, tokens, width), BF16),
            v((half, tokens, width), BF16),
            dma((4,)),
            dma((n_ep,)),
            dma((n_ep,)),
            dma((n_ep, n_tp)),
            dma((n_ep, n_tp)),
            dma((n_ep, half)),
            dma((n_ep,)),
            dma((n_ep,)),
            dma((n_ep, half)),
            dma((n_ep, half)),
            dma((n_ep,)),
            dma((n_ep,)),
            dma((2,)),
            dma((2 + 2 * n_tp,)),
        ],
        compiler_params=pltpu.CompilerParams(
            collective_id=0, has_side_effects=True, vmem_limit_bytes=60 * 1024 * 1024
        ),
    )(
        outer_gate,
        inner_gate,
        conv_input,
        conv_taps,
        mixer_weight,
        expert_input,
        norm_gain.reshape(1, -1),
        expert_ids.T,
        route_weight.T,
        gate_weight,
        up_weight,
        down_weight,
    )


def solution(mesh):
    return jax.shard_map(
        functools.partial(on_device, mesh.shape["ep"], mesh.shape["tp"]),
        mesh=mesh,
        in_specs=(
            P(("grp", "ep"), "tp"),
            P(("grp", "ep"), "tp"),
            P(("grp", "ep"), "tp"),
            P(None, "tp"),
            P("tp", None),
            P(("grp", "ep", "tp"), None),
            P(),
            P(("grp", "ep", "tp"), None),
            P(("grp", "ep", "tp"), None),
            P("ep", None, "tp"),
            P("ep", None, "tp"),
            P("ep", "tp", None),
        ),
        out_specs=(P(("grp", "ep", "tp"), None), P(("grp", "ep", "tp"), None)),
        check_vma=False,
    )
```

```python
import functools

import jax
import jax.numpy as jnp
from jax import lax
from jax.experimental import pallas as pl
from jax.experimental.pallas import tpu as pltpu
from jax.sharding import PartitionSpec as P

EPSILON = 1e-06
F32 = jnp.float32
BF16 = jnp.bfloat16
MESH = pl.DeviceIdType.MESH
HALO = 8


def round_up(value, multiple):
    return (value + multiple - 1) // multiple * multiple


def add(*values):
    total = values[0].astype(F32)
    for value in values[1:]:
        total = total + value.astype(F32)
    return total.astype(BF16)


def kernel(
    n_ep,
    n_tp,
    cap,
    outer_ref,
    inner_ref,
    conv_ref,
    taps_ref,
    mixer_hbm,
    x_ref,
    gain_ref,
    ids_ref,
    route_ref,
    gate_hbm,
    up_hbm,
    down_hbm,
    mixer_out,
    expert_out,
    mixer_w,
    gate_w,
    up_w,
    down_w,
    normed,
    weights,
    outbox,
    rows,
    part,
    core_in,
    chip_sum,
    cross_in,
    ret,
    ans,
    hid,
    gated,
    halo,
    mixed,
    m_part,
    m_core_in,
    m_chip_sum,
    m_cross_in,
    w_sem,
    z_send,
    z_recv,
    core_send,
    g_recv,
    cross_send,
    a_send,
    a_recv,
    b_send,
    b_recv,
    r_send,
    r_recv,
    h_sem,
    m_sem,
):
    half = n_tp // 2
    me = lax.axis_index("ep")
    t = lax.axis_index("tp")
    c = lax.rem(t, 2)
    a = t // 2
    pair = t + 1 - 2 * c
    others = [lax.rem(a + j, half) for j in range(1, half)]
    tokens, width = x_ref.shape
    length = inner_ref.shape[0]

    def departure(i):
        if n_ep == 4:
            if i == 0:
                return me
            two = me + 2 - 4 * (me // 2)
            if i == 1:
                return two
            one = me + 1 - 2 * lax.rem(me, 2)
            three = 3 - me
            inside = lax.rem((me + 1) // 2, 2)
            if i == 2:
                return one + inside * (three - one)
            return three + inside * (one - three)
        return lax.rem(me + i, n_ep)

    def source(i):
        if n_ep == 4:
            one = me + 1 - 2 * lax.rem(me, 2)
            inside = lax.rem((me + 1) // 2, 2)
            later = inside * (3 - me - one)
            return [me, me + 2 - 4 * (me // 2), 3 - me - later, one + later][i]
        return lax.rem(me + i, n_ep)

    def remote(src, dst, send, recv, **where):
        return pltpu.make_async_remote_copy(
            src_ref=src,
            dst_ref=dst,
            send_sem=send,
            recv_sem=recv,
            device_id=where,
            device_id_type=MESH,
        )

    loads = [
        pltpu.make_async_copy(src, dst, w_sem.at[i])
        for i, (src, dst) in enumerate(
            [
                (mixer_hbm, mixer_w),
                (gate_hbm.at[0], gate_w),
                (up_hbm.at[0], up_w),
                (down_hbm.at[0], down_w),
            ]
        )
    ]
    for load in loads:
        load.start()

    barrier = pltpu.get_barrier_semaphore()
    for j in range(1, n_ep):
        pl.semaphore_signal(
            barrier, inc=1, device_id={"ep": lax.rem(me + j, n_ep)}, device_id_type=MESH
        )
    for j in range(1, n_tp):
        pl.semaphore_signal(
            barrier, inc=1, device_id={"tp": lax.rem(t + j, n_tp)}, device_id_type=MESH
        )

    values = x_ref[...].astype(F32)
    scale = lax.rsqrt(jnp.mean(values * values, axis=1, keepdims=True) + EPSILON)
    normed[...] = (values * scale * gain_ref[...]).astype(BF16)
    e_rows = round_up(n_ep, 8)
    e_iota = lax.broadcasted_iota(jnp.int32, (e_rows, tokens), 0)
    first, second = ids_ref[0:1, :], ids_ref[1:2, :]
    is_first, is_second = e_iota == first, e_iota == second
    named = jnp.where(is_first | is_second, 1.0, 0.0).astype(BF16)
    row_i = lax.broadcasted_iota(jnp.int32, (tokens, tokens), 0)
    col_i = lax.broadcasted_iota(jnp.int32, (tokens, tokens), 1)
    before = jnp.where(row_i < col_i, 1.0, 0.0).astype(BF16)
    rank = jnp.dot(named, before, preferred_element_type=F32)
    rank_1 = jnp.sum(jnp.where(is_first, rank, 0.0), axis=0, keepdims=True)
    rank_2 = jnp.sum(jnp.where(is_second, rank, 0.0), axis=0, keepdims=True)
    slot_1 = first.astype(F32) * cap + rank_1
    slot_2 = second.astype(F32) * cap + rank_2
    slots = lax.broadcasted_iota(jnp.int32, (n_ep * cap, tokens), 0).astype(F32)
    pack = jnp.where((slots == slot_1) | (slots == slot_2), 1.0, 0.0).astype(BF16)
    tile = 512
    for n in range(width // tile):
        cols = slice(n * tile, (n + 1) * tile)
        packed = jnp.dot(pack, normed[:, cols], preferred_element_type=F32)
        outbox[:, :, cols] = packed.astype(BF16).reshape(n_ep, cap, tile)

    gated[HALO:, :] = inner_ref[...].astype(F32) * conv_ref[...].astype(F32)

    pl.semaphore_wait(barrier, n_ep - 1 + n_tp - 1)

    nxt = lax.rem(me + 1, n_ep)
    halo_copy = remote(
        gated.at[pl.ds(length, HALO)], halo, h_sem.at[0], h_sem.at[1], ep=nxt
    )
    halo_copy.start()

    def dispatch(i):
        d = departure(i)
        return remote(
            outbox.at[d], rows.at[me, t], z_send.at[d], z_recv.at[me], ep=d
        )

    def own_to_pair(s):
        return remote(
            rows.at[s, t], rows.at[s, t], core_send.at[s, t], g_recv.at[s, t], tp=pair
        )

    def own_to_cross(s, o):
        return remote(
            rows.at[s, t], rows.at[s, t], cross_send.at[s, o], g_recv.at[s, t], tp=2 * o + c
        )

    def cross_to_pair(s, o):
        q = 2 * o + c
        return remote(
            rows.at[s, q], rows.at[s, q], core_send.at[s, q], g_recv.at[s, q], tp=pair
        )

    def arrival(s, q):
        return remote(
            rows.at[s, q], rows.at[s, q], core_send.at[s, q], g_recv.at[s, q], tp=pair
        )

    def spread(s):
        for o in others:
            own_to_cross(s, o).start()
        own_to_pair(s).start()

    def pre(i):
        s = source(i)
        remote(outbox.at[s], rows.at[s, t], z_send.at[s], z_recv.at[s], ep=s).wait_recv()
        spread(s)

    def loop(lower, upper, body):
        if upper - lower <= 4:
            for i in range(lower, upper):
                body(i)
        else:
            lax.fori_loop(lower, upper, lambda i, _: (body(i), 0)[1], 0)

    rows[me, t] = outbox[me]
    spread(me)
    loop(1, n_ep, lambda i: dispatch(i).start())

    halo_copy.wait_recv()
    kept = jnp.where(me > 0, 1.0, 0.0)
    gated[0:HALO, :] = halo[...] * kept
    count = taps_ref.shape[0]
    convolved = jnp.zeros((length, gated.shape[1]), F32)
    for k in range(count):
        lower = HALO - (count - 1) + k
        convolved = convolved + taps_ref[k : k + 1, :] * gated[lower : lower + length, :]
    mixed[...] = (outer_ref[...].astype(F32) * convolved).astype(BF16)
    loads[0].wait()

    def mixer_tile(n, _):
        cols = pl.ds(pl.multiple_of(n * tile, tile), tile)
        for q in range(n_tp):
            value = jnp.dot(
                mixed[q * tokens : (q + 1) * tokens, :],
                mixer_w[:, cols],
                preferred_element_type=F32,
            )
            m_part[q % 2, q // 2, :, cols] = value.astype(BF16)
        return 0

    lax.fori_loop(0, width // tile, mixer_tile, 0)
    m_core = remote(m_part.at[1 - c], m_core_in, m_sem.at[0], m_sem.at[1], tp=pair)
    m_core.start()

    piece = tokens // 2

    def m_cross(o, h, slot):
        return remote(
            m_chip_sum.at[o, pl.ds(h * piece, piece)],
            m_cross_in.at[slot, pl.ds(h * piece, piece)],
            m_sem.at[2 + 2 * o + h],
            m_sem.at[2 + n_tp + 2 * slot + h],
            tp=2 * o + c,
        )

    m_core.wait_recv()
    for o in others:
        m_chip_sum[o] = add(m_part[c, o], m_core_in[o])
        m_cross(o, 0, a).start()

    def mixer_rest():
        for o in others:
            m_cross(o, 1, a).start()

    def mixer_finish():
        for o in others:
            m_cross(o, 0, o).wait_recv()
            m_cross(o, 1, o).wait_recv()
        mixer_out[...] = add(
            m_part[c, a], m_core_in[a], *[m_cross_in[o] for o in others]
        )

    def gathered(i):
        s = source(i)
        for o in others:
            arrival(s, 2 * o + c).wait_recv()
            cross_to_pair(s, o).start()
        for o in range(half):
            arrival(s, 2 * o + 1 - c).wait_recv()

    f_tile = 256

    def compute(i):
        s = source(i)

        def up_tile(n, _):
            cols = pl.ds(pl.multiple_of(n * f_tile, f_tile), f_tile)
            block = rows[s].reshape(n_tp * cap, width)
            g = jnp.dot(block, gate_w[:, cols], preferred_element_type=F32)
            u = jnp.dot(block, up_w[:, cols], preferred_element_type=F32)
            hid[:, cols] = (g / (1.0 + jnp.exp(-g)) * u).astype(BF16)
            return 0

        lax.fori_loop(0, hid.shape[1] // f_tile, up_tile, 0)

        def down_tile(n, _):
            cols = pl.ds(pl.multiple_of(n * tile, tile), tile)
            value = jnp.dot(hid[...], down_w[:, cols], preferred_element_type=F32)
            value = value.astype(BF16).reshape(n_tp, cap, tile)
            for q in range(n_tp):
                part[s, q % 2, q // 2, :, cols] = value[q]
            return 0

        lax.fori_loop(0, width // tile, down_tile, 0)
        to_pair(s).start()

    def to_pair(s):
        return remote(
            part.at[s, 1 - c], core_in.at[s], a_send.at[s], a_recv.at[s], tp=pair
        )

    def to_cross(s, o):
        return remote(
            chip_sum.at[s, o], cross_in.at[s, a], b_send.at[s, o], b_recv.at[s, a], tp=2 * o + c
        )

    def middle(i):
        s = source(i)
        to_pair(s).wait_recv()
        for o in others:
            chip_sum[s, o] = add(part[s, c, o], core_in[s, o])
            to_cross(s, o).start()

    def give_back(s):
        return remote(ret.at[s], ans.at[me], r_send.at[s], r_recv.at[me], ep=s)

    def finish(i, own=False):
        s = source(i)
        for o in others:
            remote(
                chip_sum.at[s, o], cross_in.at[s, o], b_send.at[s, o], b_recv.at[s, o], tp=2 * o + c
            ).wait_recv()
        total = add(part[s, c, a], core_in[s, a], *[cross_in[s, o] for o in others])
        if own:
            ans[s] = total
        else:
            ret[s] = total
            give_back(s).start()

    def step(i):
        pre(i + 1)
        gathered(i)
        compute(i)
        finish(i - 1)
        middle(i)

    for load in loads[1:]:
        load.wait()
    mixer_rest()
    pre(1)
    gathered(0)
    compute(0)
    pre(2)
    gathered(1)
    compute(1)
    middle(1)
    loop(2, n_ep - 1, step)
    gathered(n_ep - 1)
    compute(n_ep - 1)
    finish(n_ep - 2)
    middle(n_ep - 1)
    middle(0)
    mixer_finish()

    weight = jnp.where(slots == slot_1, route_ref[0:1, :], 0.0) + jnp.where(
        slots == slot_2, route_ref[1:2, :], 0.0
    )
    weights[0] = weight.astype(BF16)
    weights[1] = (weight - weight.astype(BF16).astype(F32)).astype(BF16)
    finish(n_ep - 1)
    finish(0, own=True)

    def answer_in(i):
        e = source(i)
        remote(ret.at[e], ans.at[e], r_send.at[e], r_recv.at[e], ep=e).wait_recv()

    loop(1, n_ep, answer_in)

    def weighted(left, right):
        return lax.dot_general(
            left, right, (((0,), (0,)), ((), ())), preferred_element_type=F32
        )

    def combine_tile(n, _):
        cols = pl.ds(pl.multiple_of(n * tile, tile), tile)
        block = ans[:, :, cols].reshape(n_ep * cap, tile)
        expert_out[:, cols] = (
            weighted(weights[0], block) + weighted(weights[1], block)
        ).astype(BF16)
        return 0

    lax.fori_loop(0, width // tile, combine_tile, 0)

    halo_copy.wait_send()
    m_core.wait_send()
    for o in others:
        m_cross(o, 0, a).wait_send()
        m_cross(o, 1, a).wait_send()

    def drain(i):
        s = source(i)
        for o in others:
            own_to_cross(s, o).wait_send()
            cross_to_pair(s, o).wait_send()
            to_cross(s, o).wait_send()
        own_to_pair(s).wait_send()
        to_pair(s).wait_send()

    def drain_far(i):
        dispatch(i).wait_send()
        give_back(source(i)).wait_send()

    loop(0, n_ep, drain)
    loop(1, n_ep, drain_far)


def on_device(
    n_ep,
    n_tp,
    outer_gate,
    inner_gate,
    conv_input,
    conv_taps,
    mixer_weight,
    expert_input,
    norm_gain,
    expert_ids,
    route_weight,
    gate_weight,
    up_weight,
    down_weight,
):
    tokens, width = expert_input.shape
    top = expert_ids.shape[1]
    cap = round_up(5 * tokens * top // (4 * n_ep), 16)
    half = n_tp // 2
    length, channels = inner_gate.shape
    hidden = gate_weight.shape[2]
    vmem = pl.BlockSpec(memory_space=pltpu.VMEM)
    hbm = pl.BlockSpec(memory_space=pl.ANY)
    dma = pltpu.SemaphoreType.DMA
    v = pltpu.VMEM
    out = jax.ShapeDtypeStruct((tokens, width), BF16)
    return pl.pallas_call(
        functools.partial(kernel, n_ep, n_tp, cap),
        out_shape=(out, out),
        in_specs=[vmem] * 4 + [hbm] + [vmem] * 4 + [hbm] * 3,
        out_specs=(vmem, vmem),
        scratch_shapes=[
            v(mixer_weight.shape, BF16),
            v(gate_weight.shape[1:], BF16),
            v(up_weight.shape[1:], BF16),
            v(down_weight.shape[1:], BF16),
            v((tokens, width), BF16),
            v((2, n_ep * cap, tokens), BF16),
            v((n_ep, cap, width), BF16),
            v((n_ep, n_tp, cap, width), BF16),
            v((n_ep, 2, half, cap, width), BF16),
            v((n_ep, half, cap, width), BF16),
            v((n_ep, half, cap, width), BF16),
            v((n_ep, half, cap, width), BF16),
            v((n_ep, cap, width), BF16),
            v((n_ep, cap, width), BF16),
            v((n_tp * cap, hidden), BF16),
            v((HALO + length, channels), F32),
            v((HALO, channels), F32),
            v((length, channels), BF16),
            v((2, half, tokens, width), BF16),
            v((half, tokens, width), BF16),
            v((half, tokens, width), BF16),
            v((half, tokens, width), BF16),
            dma((4,)),
            dma((n_ep,)),
            dma((n_ep,)),
            dma((n_ep, n_tp)),
            dma((n_ep, n_tp)),
            dma((n_ep, half)),
            dma((n_ep,)),
            dma((n_ep,)),
            dma((n_ep, half)),
            dma((n_ep, half)),
            dma((n_ep,)),
            dma((n_ep,)),
            dma((2,)),
            dma((2 + 2 * n_tp,)),
        ],
        compiler_params=pltpu.CompilerParams(
            collective_id=0, has_side_effects=True, vmem_limit_bytes=60 * 1024 * 1024
        ),
    )(
        outer_gate,
        inner_gate,
        conv_input,
        conv_taps,
        mixer_weight,
        expert_input,
        norm_gain.reshape(1, -1),
        expert_ids.T,
        route_weight.T,
        gate_weight,
        up_weight,
        down_weight,
    )


def solution(mesh):
    return jax.shard_map(
        functools.partial(on_device, mesh.shape["ep"], mesh.shape["tp"]),
        mesh=mesh,
        in_specs=(
            P(("grp", "ep"), "tp"),
            P(("grp", "ep"), "tp"),
            P(("grp", "ep"), "tp"),
            P(None, "tp"),
            P("tp", None),
            P(("grp", "ep", "tp"), None),
            P(),
            P(("grp", "ep", "tp"), None),
            P(("grp", "ep", "tp"), None),
            P("ep", None, "tp"),
            P("ep", None, "tp"),
            P("ep", "tp", None),
        ),
        out_specs=(P(("grp", "ep", "tp"), None), P(("grp", "ep", "tp"), None)),
        check_vma=False,
    )
```
